32 devices in a mesh: fs: 16 (over z, y, x), tp: 2 (over core).
Axes of the slice: x: 2, y: 2, z: 4, core: 2. Of those that a mesh axis runs over, the one named last changes fastest.
Arguments:
- tokens: bfloat16 [2, 256, 2048], P('tp'), may hold values from -6 to 6
- gain_first: float32 [2048], P('fs'), may hold values from 0.1 to 1.9
- gate_first: float32 [2048, 5632], P('fs', 'tp'), may hold values from -0.125 to 0.125
- up_first: float32 [2048, 5632], P('fs', 'tp'), may hold values from -0.125 to 0.125
- down_first: float32 [2048, 5632], P('fs', 'tp'), may hold values from -0.3125 to 0.3125
- gain_second: float32 [2048], P('fs'), may hold values from 0.1 to 1.9
- gate_second: float32 [2048, 5632], P('fs', 'tp'), may hold values from -0.125 to 0.125
- up_second: float32 [2048, 5632], P('fs', 'tp'), may hold values from -0.125 to 0.125
- down_second: float32 [2048, 5632], P('fs', 'tp'), may hold values from -0.3125 to 0.3125
Outputs:
- mixed: bfloat16 [2, 256, 2048], P('tp', 'fs')
- served_gate_first: bfloat16 [2, 2816, 2048], P(None, 'fs')
- served_up_first: bfloat16 [2, 2816, 2048], P(None, 'fs')
- served_down_first: bfloat16 [2, 2816, 2048], P(None, 'fs')
- served_gate_second: bfloat16 [2, 2816, 2048], P(None, 'fs')
- served_up_second: bfloat16 [2, 2816, 2048], P(None, 'fs')
- served_down_second: bfloat16 [2, 2816, 2048], P(None, 'fs')
The draws below stay inside these ranges and needn't reach their ends.
All inputs are finite; a program needn't handle non-finite values.
Results may differ from the reference program's by a relative error of at most 0.013.
Values may be sent and summed in bfloat16 or wider, within the bound.
A program may use at most 64 MiB of HBM per device.

```python
import jax
import jax.numpy as jnp
from jax import lax

D = 2048
FF = 5632
PLEN = 256
PROMPTS = 2
N_TP = 2


def steps_of(key, dims, pieces, smallest, largest):
    loudness = 1.0
    for position, blocks in pieces:
        draws = jax.random.uniform(jax.random.fold_in(jax.random.fold_in(key, 6), position), (blocks,), jnp.float32, smallest / len(pieces), largest / len(pieces))
        loudness = loudness * jnp.repeat(jnp.exp(draws), dims[position] // blocks).reshape((-1,) + (1,) * (len(dims) - 1 - position))
    return loudness


def bell_draw(rng, dims, width, reach, split=(), kind=jnp.bfloat16):
    values = jax.random.normal(rng, dims, jnp.float32) * width
    if len(split) > 0:
        values = steps_of(rng, dims, split, -0.22, 0.18) * values
    return jnp.clip(values, min=-reach, max=reach).astype(kind)


def setup_inputs(seed: int = 0) -> dict:
    keys = jax.random.split(jax.random.key(seed), 10)
    tokens = bell_draw(keys[0], (PROMPTS, PLEN, D), 1.0, 6.0, ((0, 2),))
    gain_first = jnp.clip(1.0 + 0.18 * jax.random.normal(keys[1], (D,), jnp.float32), 0.1, 1.9)
    gate_first = bell_draw(keys[2], (D, FF), D ** -0.5, 0.125, ((0, 16), (1, 2)), jnp.float32)
    up_first = bell_draw(keys[3], (D, FF), D ** -0.5, 0.125, ((0, 16), (1, 2)), jnp.float32)
    down_first = bell_draw(keys[4], (D, FF), (FF // 16) ** -0.5, 0.3125, ((0, 16), (1, 2)), jnp.float32)
    gain_second = jnp.clip(1.0 + 0.18 * jax.random.normal(keys[5], (D,), jnp.float32), 0.1, 1.9)
    gate_second = bell_draw(keys[6], (D, FF), D ** -0.5, 0.125, ((0, 16), (1, 2)), jnp.float32)
    up_second = bell_draw(keys[7], (D, FF), D ** -0.5, 0.125, ((0, 16), (1, 2)), jnp.float32)
    down_second = bell_draw(keys[8], (D, FF), (FF // 16) ** -0.5, 0.3125, ((0, 16), (1, 2)), jnp.float32)
    return {"tokens": tokens, "gain_first": gain_first, "gate_first": gate_first, "up_first": up_first, "down_first": down_first, "gain_second": gain_second, "gate_second": gate_second, "up_second": up_second, "down_second": down_second}


def normalize(values):
    wide = values.astype(jnp.float32)
    scale = lax.rsqrt(lax.optimization_barrier(jnp.mean(wide * wide, axis=-1, keepdims=True)) + 1e-06)
    return (wide * scale).astype(jnp.bfloat16)

def gated_branch(values, gate_cast, up_cast, down_cast):
    normed = normalize(values)
    gate_act = jnp.dot(normed, gate_cast, preferred_element_type=jnp.float32)
    up_act = jnp.dot(normed, up_cast, preferred_element_type=jnp.float32)
    hidden = (jax.nn.silu(gate_act) * up_act).astype(jnp.bfloat16)
    return jnp.dot(hidden, down_cast.T, preferred_element_type=jnp.float32)

def served(cast):
    return cast.T.reshape(N_TP, FF // N_TP, D)

def reference(tokens, gain_first, gate_first, up_first, down_first, gain_second, gate_second, up_second, down_second):
    gate_one = (gate_first * gain_first[:, None]).astype(jnp.bfloat16)
    up_one = (up_first * gain_first[:, None]).astype(jnp.bfloat16)
    down_one = down_first.astype(jnp.bfloat16)
    gate_two = (gate_second * gain_second[:, None]).astype(jnp.bfloat16)
    up_two = (up_second * gain_second[:, None]).astype(jnp.bfloat16)
    down_two = down_second.astype(jnp.bfloat16)
    rows = tokens.reshape(-1, D)
    branch_first = gated_branch(rows, gate_one, up_one, down_one)
    middle = (rows.astype(jnp.float32) + 0.5 * branch_first).astype(jnp.bfloat16)
    branch_second = gated_branch(middle, gate_two, up_two, down_two)
    mixed = (middle.astype(jnp.float32) + 0.5 * branch_second).astype(jnp.bfloat16)
    return (mixed.reshape(tokens.shape), served(gate_one), served(up_one), served(down_one), served(gate_two), served(up_two), served(down_two))
```

```python
import functools
import math

import jax
import jax.numpy as jnp
from jax import lax
from jax.experimental import pallas as pl
from jax.experimental.pallas import tpu as pltpu
from jax.sharding import PartitionSpec as P


def normalize(values):
    wide = values.astype(jnp.float32)
    scale = lax.rsqrt(jnp.mean(wide * wide, axis=-1, keepdims=True) + 1e-06)
    return (wide * scale).astype(jnp.bfloat16)


def folded(weight, gain):
    return (weight * gain[:, None]).astype(jnp.bfloat16).T


def relayout(gate_part, up_part, down_part):
    gate_cut, up_cut, down_cut = (
        lax.all_to_all(gate_part, "fs", split_axis=0, concat_axis=1, tiled=True),
        lax.all_to_all(up_part, "fs", split_axis=0, concat_axis=1, tiled=True),
        lax.all_to_all(down_part, "fs", split_axis=0, concat_axis=1, tiled=True),
    )
    return (
        lax.all_gather(gate_cut[None], "tp", axis=0, tiled=True),
        lax.all_gather(up_cut[None], "tp", axis=0, tiled=True),
        lax.all_gather(down_cut[None], "tp", axis=0, tiled=True),
    )


def hidden_of(normed, gate_served, up_served):
    gate_flat = gate_served.reshape(-1, gate_served.shape[2])
    up_flat = up_served.reshape(-1, up_served.shape[2])
    gate_act = jnp.einsum("rd,hd->rh", normed, gate_flat, preferred_element_type=jnp.float32)
    up_act = jnp.einsum("rd,hd->rh", normed, up_flat, preferred_element_type=jnp.float32)
    return (jax.nn.silu(gate_act) * up_act).astype(jnp.bfloat16)


def projector(hidden, down_flat):
    return jnp.dot(hidden, down_flat, preferred_element_type=jnp.float32)


def shards(
    tokens,
    gain_first,
    gate_first,
    up_first,
    down_first,
    gain_second,
    gate_second,
    up_second,
    down_second,
):
    gate_one, up_one, down_one = relayout(
        folded(gate_first, gain_first),
        folded(up_first, gain_first),
        down_first.astype(jnp.bfloat16).T,
    )
    gate_two, up_two, down_two = relayout(
        folded(gate_second, gain_second),
        folded(up_second, gain_second),
        down_second.astype(jnp.bfloat16).T,
    )
    rows = tokens[0]
    keep = rows.shape[0] // lax.axis_size("fs")
    offset = lax.axis_index("fs") * keep
    hidden_first = hidden_of(normalize(rows), gate_one, up_one)
    down_flat_one = down_one.reshape(-1, down_one.shape[2])
    partial_value = jnp.dot(hidden_first, down_flat_one, preferred_element_type=jnp.float32)
    branch = lax.psum(partial_value, "fs")
    whole_middle = (rows.astype(jnp.float32) + 0.5 * branch).astype(jnp.bfloat16)
    hidden_second = hidden_of(normalize(whole_middle), gate_two, up_two)
    middle = lax.dynamic_slice_in_dim(whole_middle, offset, keep, 0)
    down_flat_two = down_two.reshape(-1, down_two.shape[2])
    branch_two = lax.psum_scatter(
        projector(hidden_second, down_flat_two), "fs", scatter_dimension=0, tiled=True
    )
    mixed = (middle.astype(jnp.float32) + 0.5 * branch_two).astype(jnp.bfloat16)[None]
    return (mixed, gate_one, up_one, down_one, gate_two, up_two, down_two)


def loop(lo, hi, body):
    lax.fori_loop(lo, hi, lambda i, c: (body(i), c)[1], 0)


def step_kernel(
    n,
    inner,
    tokens_ref,
    gain_one_ref,
    gain_two_ref,
    w0,
    w1,
    w2,
    w3,
    w4,
    w5,
    mixed_ref,
    o0,
    o1,
    o2,
    o3,
    o4,
    o5,
    raw,
    cut,
    served,
    normed,
    gate_acc,
    up_acc,
    hidden,
    middle,
    part,
    plane_in,
    plane_sum,
    line_in,
    load_sem,
    store_sem,
    send_sem,
    recv_sem,
    pass_send,
    pass_recv,
    ring_send,
    ring_recv,
):
    outer = n // inner
    me = lax.axis_index("fs")
    core = lax.axis_index("tp")
    row = me // inner
    col = lax.rem(me, inner)
    weights = (w0, w1, w2, w3, w4, w5)
    outs = (o0, o1, o2, o3, o4, o5)
    rows = served.shape[2]
    feats = cut.shape[2]
    depth = normed.shape[1]
    mine = pl.ds(pl.multiple_of(me * feats, feats), feats)

    def load(a):
        return pltpu.make_async_copy(weights[a], raw.at[a], load_sem.at[a])

    def store(a):
        return pltpu.make_async_copy(served.at[a], outs[a], store_sem.at[a])

    def cast(a):
        load(a).wait()
        gain = gain_one_ref if a < 3 else gain_two_ref

        def tile(i):
            at = pl.ds(pl.multiple_of(i * 128, 128), 128)
            block = raw[a, :, at].T
            if a % 3 != 2:
                block = block * gain[...]
            cut[a, at, :] = block.astype(jnp.bfloat16)

        loop(0, raw.shape[2] // 128, tile)
        served[a, core, :, mine] = cut[a, pl.ds(pl.multiple_of(me * rows, rows), rows), :]

    def block_copy(a, j):
        k = lax.rem(j, outer) * inner + j // outer
        to = lax.rem(me + k, n)
        return pltpu.make_async_remote_copy(
            src_ref=cut.at[a, pl.ds(pl.multiple_of(to * rows, rows), rows), :],
            dst_ref=served.at[a, core, :, mine],
            send_sem=send_sem.at[a, j],
            recv_sem=recv_sem.at[a, j],
            device_id={"fs": to},
            device_id_type=pl.DeviceIdType.MESH,
        )

    def send(a):
        loop(1, n, lambda j: block_copy(a, j).start())

    def pass_copy(a):
        return pltpu.make_async_remote_copy(
            src_ref=served.at[a, core],
            dst_ref=served.at[a, core],
            send_sem=pass_send.at[a],
            recv_sem=pass_recv.at[a],
            device_id={"tp": 1 - core},
            device_id_type=pl.DeviceIdType.MESH,
        )

    def arrive(a):
        loop(1, n, lambda j: block_copy(a, j).wait_recv())
        pass_copy(a).start()

    def complete(a):
        pass_copy(a).wait_recv()
        store(a).start()

    def ring_copy(stage, k, src, dst, to):
        return pltpu.make_async_remote_copy(
            src_ref=src,
            dst_ref=dst,
            send_sem=ring_send.at[stage, k],
            recv_sem=ring_recv.at[stage, k],
            device_id={"fs": to},
            device_id_type=pl.DeviceIdType.MESH,
        )

    def plane_copies(half):
        copies = []
        for k in range(1, inner):
            to = lax.rem(col + k, inner)
            copies.append(
                ring_copy(half, k, part.at[half, to], plane_in.at[half, k - 1], row * inner + to)
            )
        return copies

    def line_copies(half):
        copies = []
        for k in range(1, outer):
            to = lax.rem(row + k, outer)
            copies.append(
                ring_copy(
                    2 + half, k, plane_sum.at[half, to], line_in.at[half, k - 1], to * inner + col
                )
            )
        return copies

    def spread_line():
        spot = middle.at[col, row]
        return [
            ring_copy(4, k, spot, spot, lax.rem(row + k, outer) * inner + col)
            for k in range(1, outer)
        ]

    def spread_plane():
        spot = middle.at[col]
        return [
            ring_copy(5, k, spot, spot, row * inner + lax.rem(col + k, inner))
            for k in range(1, inner)
        ]

    keep = tokens_ref.shape[2]

    def normalize_rows(source):
        def one(i):
            wide = source[i // outer, lax.rem(i, outer)].astype(jnp.float32)
            scale = lax.rsqrt(jnp.mean(wide * wide, axis=-1, keepdims=True) + 1e-06)
            at = pl.ds(pl.multiple_of(i * keep, keep), keep)
            normed[at, :] = (wide * scale).astype(jnp.bfloat16)

        loop(0, n, one)

    def expand(g, u):
        gate_acc[...] = jnp.zeros_like(gate_acc)
        up_acc[...] = jnp.zeros_like(up_acc)
        wide = 256

        def one(i):
            at = pl.ds(pl.multiple_of(i * wide, wide), wide)
            left = normed[:, at]
            for acc, a in ((gate_acc, g), (up_acc, u)):
                right = served[a, :, :, at].reshape(-1, wide)
                acc[...] += lax.dot_general(
                    left, right, (((1,), (1,)), ((), ())), preferred_element_type=jnp.float32
                )

        loop(0, depth // wide, one)
        gate = gate_acc[...]
        hidden[...] = (gate / (1.0 + jnp.exp(-gate)) * up_acc[...]).astype(jnp.bfloat16)

    def contract(d, half):
        wide = 256

        def one(i):
            at = pl.ds(pl.multiple_of(i * wide, wide), wide)
            right = served[d, :, :, at].reshape(-1, wide)
            value = jnp.dot(hidden[...], right, preferred_element_type=jnp.float32)
            part[half, :, :, :, at] = value.astype(jnp.bfloat16).reshape(inner, outer, keep, wide)

        loop(0, depth // wide, one)

    def sum_plane(half):
        def one(i):
            total = part[half, col, i].astype(jnp.float32)
            for k in range(inner - 1):
                total += plane_in[half, k, i].astype(jnp.float32)
            plane_sum[half, i] = total.astype(jnp.bfloat16)

        loop(0, outer, one)

    def sum_line(half):
        total = plane_sum[half, row].astype(jnp.float32)
        for k in range(outer - 1):
            total += line_in[half, k].astype(jnp.float32)
        return total

    def start(copies):
        for copy in copies:
            copy.start()

    def receive(copies):
        for copy in copies:
            copy.wait_recv()

    for a in range(6):
        load(a).start()
    for a in range(4):
        cast(a)
        send(a)
    cast(4)
    cast(5)
    normalize_rows(tokens_ref)
    arrive(0)
    arrive(1)
    complete(0)
    complete(1)
    expand(0, 1)
    arrive(2)
    complete(2)
    contract(2, 0)
    start(plane_copies(0))
    send(4)
    receive(plane_copies(0))
    sum_plane(0)
    start(line_copies(0))
    receive(line_copies(0))
    own = tokens_ref[col, row].astype(jnp.float32) + 0.5 * sum_line(0)
    middle[col, row] = own.astype(jnp.bfloat16)
    start(spread_line())
    receive(spread_line())
    start(spread_plane())
    send(5)
    arrive(3)
    receive(spread_plane())
    normalize_rows(middle)
    arrive(4)
    complete(3)
    complete(4)
    expand(3, 4)
    arrive(5)
    complete(5)
    contract(5, 1)
    start(plane_copies(1))
    receive(plane_copies(1))
    sum_plane(1)
    start(line_copies(1))
    receive(line_copies(1))
    last = middle[col, row].astype(jnp.float32) + 0.5 * sum_line(1)
    mixed_ref[...] = last.astype(jnp.bfloat16)

    for a in range(6):
        store(a).wait()
        pass_copy(a).wait_send()
        loop(1, n, lambda j, a=a: block_copy(a, j).wait_send())
    for copies in (
        plane_copies(0),
        plane_copies(1),
        line_copies(0),
        line_copies(1),
        spread_line(),
        spread_plane(),
    ):
        for copy in copies:
            copy.wait_send()


def hand_on(*refs):
    half = len(refs) // 2
    for source, target in zip(refs[:half], refs[half:]):
        target[...] = source[...]


def fused_shards(tokens, gain_first, gate_first, up_first, down_first,
                 gain_second, gate_second, up_second, down_second):
    n = lax.axis_size("fs")
    tp = lax.axis_size("tp")
    inner = math.isqrt(n)
    outer = n // inner
    feats, units = gate_first.shape
    rows = units // n
    plen, depth = tokens.shape[1], tokens.shape[2]
    keep = plen // n
    bf16, f32 = jnp.bfloat16, jnp.float32
    shuffled = tokens[0].reshape(outer, inner, keep, depth).transpose(1, 0, 2, 3)
    vmem = pl.BlockSpec(memory_space=pltpu.VMEM)
    anywhere = pl.BlockSpec(memory_space=pl.ANY)
    served_shape = jax.ShapeDtypeStruct((tp, rows, depth), bf16)
    hid = tp * rows
    dma = pltpu.SemaphoreType.DMA
    width = max(inner, outer)
    results = pl.pallas_call(
        functools.partial(step_kernel, n, inner),
        out_shape=(jax.ShapeDtypeStruct((keep, depth), bf16),) + (served_shape,) * 6,
        in_specs=[vmem] * 3 + [anywhere] * 6,
        out_specs=(vmem,) + (anywhere,) * 6,
        scratch_shapes=[
            pltpu.VMEM((6, feats, units), f32),
            pltpu.VMEM((6, units, feats), bf16),
            pltpu.VMEM((6, tp, rows, depth), bf16),
            pltpu.VMEM((plen, depth), bf16),
            pltpu.VMEM((plen, hid), f32),
            pltpu.VMEM((plen, hid), f32),
            pltpu.VMEM((plen, hid), bf16),
            pltpu.VMEM((inner, outer, keep, depth), bf16),
            pltpu.VMEM((2, inner, outer, keep, depth), bf16),
            pltpu.VMEM((2, inner - 1, outer, keep, depth), bf16),
            pltpu.VMEM((2, outer, keep, depth), bf16),
            pltpu.VMEM((2, outer - 1, keep, depth), bf16),
            dma((6,)),
            dma((6,)),
            dma((6, n)),
            dma((6, n)),
            dma((6,)),
            dma((6,)),
            dma((6, width)),
            dma((6, width)),
        ],
        compiler_params=pltpu.CompilerParams(
            has_side_effects=True, vmem_limit_bytes=58 * 1024 * 1024
        ),
    )(
        shuffled,
        gain_first.reshape(1, feats),
        gain_second.reshape(1, feats),
        gate_first,
        up_first,
        down_first,
        gate_second,
        up_second,
        down_second,
    )
    block = pl.BlockSpec((1, rows, depth // 2), lambda i, j: (i, 0, j))
    copies = pl.pallas_call(
        hand_on,
        grid=(tp, 2),
        out_shape=(served_shape,) * 6,
        in_specs=[block] * 6,
        out_specs=(block,) * 6,
    )(*results[1:])
    return (results[0][None],) + tuple(copies)


def fits(mesh, tokens, gate):
    n, tp = mesh.shape["fs"], mesh.shape["tp"]
    inner = math.isqrt(n)
    depth, hidden = gate.shape
    plen = tokens.shape[1]
    if tp != 2 or inner < 2 or n % inner or depth % (n * 128) or hidden % (tp * n * 16):
        return False
    if depth % 256 or (hidden // tp) % 128 or plen % (n * 16) or tokens.shape[0] != tp:
        return False
    local = depth // n * (hidden // tp)
    need = local * 6 * 4 + local * 6 * 2 + local * 6 * 2 * tp
    need += plen * depth * 2 * 10 + plen * (hidden // n) * 12
    return need < 40 * 1024 * 1024


def solution(mesh):
    def run(body):
        return jax.shard_map(
            body,
            mesh=mesh,
            in_specs=(
                P("tp", None, None),
                P("fs"),
                P("fs", "tp"),
                P("fs", "tp"),
                P("fs", "tp"),
                P("fs"),
                P("fs", "tp"),
                P("fs", "tp"),
                P("fs", "tp"),
            ),
            out_specs=(
                P("tp", "fs", None),
                P(None, "fs", None),
                P(None, "fs", None),
                P(None, "fs", None),
                P(None, "fs", None),
                P(None, "fs", None),
                P(None, "fs", None),
            ),
            check_vma=False,
        )

    def step(*args):
        return run(fused_shards if fits(mesh, args[0], args[2]) else shards)(*args)

    return step
```

```python
import functools
import math

import jax
import jax.numpy as jnp
from jax import lax
from jax.experimental import pallas as pl
from jax.experimental.pallas import tpu as pltpu
from jax.sharding import PartitionSpec as P


def normalize(values):
    wide = values.astype(jnp.float32)
    scale = lax.rsqrt(jnp.mean(wide * wide, axis=-1, keepdims=True) + 1e-06)
    return (wide * scale).astype(jnp.bfloat16)


def folded(weight, gain):
    return (weight * gain[:, None]).astype(jnp.bfloat16).T


def relayout(gate_part, up_part, down_part):
    gate_cut, up_cut, down_cut = (
        lax.all_to_all(gate_part, "fs", split_axis=0, concat_axis=1, tiled=True),
        lax.all_to_all(up_part, "fs", split_axis=0, concat_axis=1, tiled=True),
        lax.all_to_all(down_part, "fs", split_axis=0, concat_axis=1, tiled=True),
    )
    return (
        lax.all_gather(gate_cut[None], "tp", axis=0, tiled=True),
        lax.all_gather(up_cut[None], "tp", axis=0, tiled=True),
        lax.all_gather(down_cut[None], "tp", axis=0, tiled=True),
    )


def hidden_of(normed, gate_served, up_served):
    gate_flat = gate_served.reshape(-1, gate_served.shape[2])
    up_flat = up_served.reshape(-1, up_served.shape[2])
    gate_act = jnp.einsum("rd,hd->rh", normed, gate_flat, preferred_element_type=jnp.float32)
    up_act = jnp.einsum("rd,hd->rh", normed, up_flat, preferred_element_type=jnp.float32)
    return (jax.nn.silu(gate_act) * up_act).astype(jnp.bfloat16)


def projector(hidden, down_flat):
    return jnp.dot(hidden, down_flat, preferred_element_type=jnp.float32)


def shards(
    tokens,
    gain_first,
    gate_first,
    up_first,
    down_first,
    gain_second,
    gate_second,
    up_second,
    down_second,
):
    gate_one, up_one, down_one = relayout(
        folded(gate_first, gain_first),
        folded(up_first, gain_first),
        down_first.astype(jnp.bfloat16).T,
    )
    gate_two, up_two, down_two = relayout(
        folded(gate_second, gain_second),
        folded(up_second, gain_second),
        down_second.astype(jnp.bfloat16).T,
    )
    rows = tokens[0]
    keep = rows.shape[0] // lax.axis_size("fs")
    offset = lax.axis_index("fs") * keep
    hidden_first = hidden_of(normalize(rows), gate_one, up_one)
    down_flat_one = down_one.reshape(-1, down_one.shape[2])
    partial_value = jnp.dot(hidden_first, down_flat_one, preferred_element_type=jnp.float32)
    branch = lax.psum(partial_value, "fs")
    whole_middle = (rows.astype(jnp.float32) + 0.5 * branch).astype(jnp.bfloat16)
    hidden_second = hidden_of(normalize(whole_middle), gate_two, up_two)
    middle = lax.dynamic_slice_in_dim(whole_middle, offset, keep, 0)
    down_flat_two = down_two.reshape(-1, down_two.shape[2])
    branch_two = lax.psum_scatter(
        projector(hidden_second, down_flat_two), "fs", scatter_dimension=0, tiled=True
    )
    mixed = (middle.astype(jnp.float32) + 0.5 * branch_two).astype(jnp.bfloat16)[None]
    return (mixed, gate_one, up_one, down_one, gate_two, up_two, down_two)


def loop(lo, hi, body):
    lax.fori_loop(lo, hi, lambda i, c: (body(i), c)[1], 0)


def step_kernel(
    n,
    inner,
    tokens_ref,
    gain_one_ref,
    gain_two_ref,
    w0,
    w1,
    w2,
    w3,
    w4,
    w5,
    mixed_ref,
    o0,
    o1,
    o2,
    o3,
    o4,
    o5,
    raw,
    cut,
    served,
    normed,
    gate_acc,
    up_acc,
    hidden,
    middle,
    part,
    plane_in,
    plane_sum,
    line_in,
    load_sem,
    store_sem,
    send_sem,
    recv_sem,
    pass_send,
    pass_recv,
    ring_send,
    ring_recv,
):
    outer = n // inner
    me = lax.axis_index("fs")
    core = lax.axis_index("tp")
    row = me // inner
    col = lax.rem(me, inner)
    weights = (w0, w1, w2, w3, w4, w5)
    outs = (o0, o1, o2, o3, o4, o5)
    rows = served.shape[2]
    feats = cut.shape[2]
    depth = normed.shape[1]
    mine = pl.ds(pl.multiple_of(me * feats, feats), feats)

    def load(a):
        return pltpu.make_async_copy(weights[a], raw.at[a], load_sem.at[a])

    def store(a):
        return pltpu.make_async_copy(served.at[a], outs[a], store_sem.at[a])

    def cast(a):
        load(a).wait()
        gain = gain_one_ref if a < 3 else gain_two_ref

        count = raw.shape[2] // 128
        per = next(d for d in (11, 4, 2, 1) if count % d == 0)
        spread = jnp.broadcast_to(gain[...], (128, feats)).T

        def tile(i):
            for piece in range(per):
                at = pl.ds(pl.multiple_of((i * per + piece) * 128, 128), 128)
                block = raw[a, :, at]
                if a % 3 != 2:
                    block = block * spread
                cut[a, at, :] = block.astype(jnp.bfloat16).T

        loop(0, count // per, tile)
        served[a, core, :, mine] = cut[a, pl.ds(pl.multiple_of(me * rows, rows), rows), :]

    def block_copy(a, j):
        k = lax.rem(j, outer) * inner + j // outer
        to = lax.rem(me + k, n)
        return pltpu.make_async_remote_copy(
            src_ref=cut.at[a, pl.ds(pl.multiple_of(to * rows, rows), rows), :],
            dst_ref=served.at[a, core, :, mine],
            send_sem=send_sem.at[a, j],
            recv_sem=recv_sem.at[a, j],
            device_id={"fs": to},
            device_id_type=pl.DeviceIdType.MESH,
        )

    def send(a):
        loop(1, n, lambda j: block_copy(a, j).start())

    def pass_copy(a):
        return pltpu.make_async_remote_copy(
            src_ref=served.at[a, core],
            dst_ref=served.at[a, core],
            send_sem=pass_send.at[a],
            recv_sem=pass_recv.at[a],
            device_id={"tp": 1 - core},
            device_id_type=pl.DeviceIdType.MESH,
        )

    def arrive(a):
        loop(1, n, lambda j: block_copy(a, j).wait_recv())
        pass_copy(a).start()

    def complete(a):
        pass_copy(a).wait_recv()
        store(a).start()

    def ring_copy(stage, k, src, dst, to):
        return pltpu.make_async_remote_copy(
            src_ref=src,
            dst_ref=dst,
            send_sem=ring_send.at[stage, k],
            recv_sem=ring_recv.at[stage, k],
            device_id={"fs": to},
            device_id_type=pl.DeviceIdType.MESH,
        )

    def plane_copies(half):
        copies = []
        for k in range(1, inner):
            to = lax.rem(col + k, inner)
            copies.append(
                ring_copy(half, k, part.at[half, to], plane_in.at[half, k - 1], row * inner + to)
            )
        return copies

    def line_copies(half):
        copies = []
        for k in range(1, outer):
            to = lax.rem(row + k, outer)
            copies.append(
                ring_copy(
                    2 + half, k, plane_sum.at[half, to], line_in.at[half, k - 1], to * inner + col
                )
            )
        return copies

    def spread_line():
        spot = middle.at[col, row]
        return [
            ring_copy(4, k, spot, spot, lax.rem(row + k, outer) * inner + col)
            for k in range(1, outer)
        ]

    def spread_plane():
        spot = middle.at[col]
        return [
            ring_copy(5, k, spot, spot, row * inner + lax.rem(col + k, inner))
            for k in range(1, inner)
        ]

    keep = tokens_ref.shape[2]

    def normalize_rows(pick):
        def one(i):
            wide = pick(i // outer, lax.rem(i, outer)).astype(jnp.float32)
            scale = lax.rsqrt(jnp.mean(wide * wide, axis=-1, keepdims=True) + 1e-06)
            at = pl.ds(pl.multiple_of(i * keep, keep), keep)
            normed[at, :] = (wide * scale).astype(jnp.bfloat16)

        loop(0, n, one)

    def expand(g, u):
        gate_acc[...] = jnp.zeros_like(gate_acc)
        up_acc[...] = jnp.zeros_like(up_acc)
        wide = 256

        def one(i):
            at = pl.ds(pl.multiple_of(i * wide, wide), wide)
            left = normed[:, at]
            for acc, a in ((gate_acc, g), (up_acc, u)):
                right = served[a, :, :, at].reshape(-1, wide)
                acc[...] += lax.dot_general(
                    left, right, (((1,), (1,)), ((), ())), preferred_element_type=jnp.float32
                )

        loop(0, depth // wide, one)
        gate = gate_acc[...]
        hidden[...] = (gate / (1.0 + jnp.exp(-gate)) * up_acc[...]).astype(jnp.bfloat16)

    def contract(d, half):
        wide = 256

        def one(i):
            at = pl.ds(pl.multiple_of(i * wide, wide), wide)
            right = served[d, :, :, at].reshape(-1, wide)
            value = jnp.dot(hidden[...], right, preferred_element_type=jnp.float32)
            part[half, :, :, :, at] = value.astype(jnp.bfloat16).reshape(inner, outer, keep, wide)

        loop(0, depth // wide, one)

    def sum_plane(half):
        def one(i):
            total = part[half, col, i].astype(jnp.float32)
            for k in range(inner - 1):
                total += plane_in[half, k, i].astype(jnp.float32)
            plane_sum[half, i] = total.astype(jnp.bfloat16)

        loop(0, outer, one)

    def sum_line(half):
        total = plane_sum[half, row].astype(jnp.float32)
        for k in range(outer - 1):
            total += line_in[half, k].astype(jnp.float32)
        return total

    def start(copies):
        for copy in copies:
            copy.start()

    def receive(copies):
        for copy in copies:
            copy.wait_recv()

    for a in range(6):
        load(a).start()
    for a in range(4):
        cast(a)
        send(a)
    cast(4)
    cast(5)
    normalize_rows(lambda c, r: tokens_ref[r, c])
    arrive(0)
    arrive(1)
    complete(0)
    complete(1)
    expand(0, 1)
    arrive(2)
    complete(2)
    contract(2, 0)
    start(plane_copies(0))
    send(4)
    receive(plane_copies(0))
    sum_plane(0)
    start(line_copies(0))
    receive(line_copies(0))
    own = tokens_ref[row, col].astype(jnp.float32) + 0.5 * sum_line(0)
    middle[col, row] = own.astype(jnp.bfloat16)
    start(spread_line())
    receive(spread_line())
    start(spread_plane())
    send(5)
    arrive(3)
    receive(spread_plane())
    normalize_rows(lambda c, r: middle[c, r])
    arrive(4)
    complete(3)
    complete(4)
    expand(3, 4)
    arrive(5)
    complete(5)
    contract(5, 1)
    start(plane_copies(1))
    receive(plane_copies(1))
    sum_plane(1)
    start(line_copies(1))
    receive(line_copies(1))
    last = middle[col, row].astype(jnp.float32) + 0.5 * sum_line(1)
    mixed_ref[...] = last.astype(jnp.bfloat16)

    for a in range(6):
        store(a).wait()
        pass_copy(a).wait_send()
        loop(1, n, lambda j, a=a: block_copy(a, j).wait_send())
    for copies in (
        plane_copies(0),
        plane_copies(1),
        line_copies(0),
        line_copies(1),
        spread_line(),
        spread_plane(),
    ):
        for copy in copies:
            copy.wait_send()


def hand_on(*refs):
    half = len(refs) // 2
    for source, target in zip(refs[:half], refs[half:]):
        target[...] = source[...]


def fused_shards(tokens, gain_first, gate_first, up_first, down_first,
                 gain_second, gate_second, up_second, down_second):
    n = lax.axis_size("fs")
    tp = lax.axis_size("tp")
    inner = math.isqrt(n)
    outer = n // inner
    feats, units = gate_first.shape
    rows = units // n
    plen, depth = tokens.shape[1], tokens.shape[2]
    keep = plen // n
    bf16, f32 = jnp.bfloat16, jnp.float32
    shuffled = tokens[0].reshape(outer, inner, keep, depth)
    vmem = pl.BlockSpec(memory_space=pltpu.VMEM)
    anywhere = pl.BlockSpec(memory_space=pl.ANY)
    served_shape = jax.ShapeDtypeStruct((tp, rows, depth), bf16)
    hid = tp * rows
    dma = pltpu.SemaphoreType.DMA
    width = max(inner, outer)
    results = pl.pallas_call(
        functools.partial(step_kernel, n, inner),
        out_shape=(jax.ShapeDtypeStruct((keep, depth), bf16),) + (served_shape,) * 6,
        in_specs=[vmem] * 3 + [anywhere] * 6,
        out_specs=(vmem,) + (anywhere,) * 6,
        scratch_shapes=[
            pltpu.VMEM((6, feats, units), f32),
            pltpu.VMEM((6, units, feats), bf16),
            pltpu.VMEM((6, tp, rows, depth), bf16),
            pltpu.VMEM((plen, depth), bf16),
            pltpu.VMEM((plen, hid), f32),
            pltpu.VMEM((plen, hid), f32),
            pltpu.VMEM((plen, hid), bf16),
            pltpu.VMEM((inner, outer, keep, depth), bf16),
            pltpu.VMEM((2, inner, outer, keep, depth), bf16),
            pltpu.VMEM((2, inner - 1, outer, keep, depth), bf16),
            pltpu.VMEM((2, outer, keep, depth), bf16),
            pltpu.VMEM((2, outer - 1, keep, depth), bf16),
            dma((6,)),
            dma((6,)),
            dma((6, n)),
            dma((6, n)),
            dma((6,)),
            dma((6,)),
            dma((6, width)),
            dma((6, width)),
        ],
        compiler_params=pltpu.CompilerParams(
            has_side_effects=True, vmem_limit_bytes=58 * 1024 * 1024
        ),
    )(
        shuffled,
        gain_first.reshape(1, feats),
        gain_second.reshape(1, feats),
        gate_first,
        up_first,
        down_first,
        gate_second,
        up_second,
        down_second,
    )
    block = pl.BlockSpec((1, rows, depth // 2), lambda i, j: (i, 0, j))
    copies = pl.pallas_call(
        hand_on,
        grid=(tp, 2),
        out_shape=(served_shape,) * 6,
        in_specs=[block] * 6,
        out_specs=(block,) * 6,
    )(*results[1:])
    return (results[0][None],) + tuple(copies)


def fits(mesh, tokens, gate):
    n, tp = mesh.shape["fs"], mesh.shape["tp"]
    inner = math.isqrt(n)
    depth, hidden = gate.shape
    plen = tokens.shape[1]
    if tp != 2 or inner < 2 or n % inner or depth % (n * 128) or hidden % (tp * n * 16):
        return False
    if depth % 256 or (hidden // tp) % 128 or plen % (n * 16) or tokens.shape[0] != tp:
        return False
    local = depth // n * (hidden // tp)
    need = local * 6 * 4 + local * 6 * 2 + local * 6 * 2 * tp
    need += plen * depth * 2 * 10 + plen * (hidden // n) * 12
    return need < 40 * 1024 * 1024


def solution(mesh):
    def run(body):
        return jax.shard_map(
            body,
            mesh=mesh,
            in_specs=(
                P("tp", None, None),
                P("fs"),
                P("fs", "tp"),
                P("fs", "tp"),
                P("fs", "tp"),
                P("fs"),
                P("fs", "tp"),
                P("fs", "tp"),
                P("fs", "tp"),
            ),
            out_specs=(
                P("tp", "fs", None),
                P(None, "fs", None),
                P(None, "fs", None),
                P(None, "fs", None),
                P(None, "fs", None),
                P(None, "fs", None),
                P(None, "fs", None),
            ),
            check_vma=False,
        )

    def step(*args):
        return run(fused_shards if fits(mesh, args[0], args[2]) else shards)(*args)

    return step
```
